32 devices in a mesh: rep: 2 (over x), fs: 8 (over z, y), tp: 2 (over core).
Axes of the slice: x: 2, y: 2, z: 4, core: 2. Of those that a mesh axis runs over, the one named last changes fastest.
Arguments:
- stream: bfloat16 [4096, 2048], P(('rep', 'fs'), 'tp'), may hold values from -6 to 6
- norm_gains: float32 [6, 2048], replicated, may hold values from 0.1 to 1.9
- w_gate: bfloat16 [2048, 5632], P('fs', 'tp'), may hold values from -0.125 to 0.125
- w_up: bfloat16 [2048, 5632], P('fs', 'tp'), may hold values from -0.125 to 0.125
- w_down: bfloat16 [5632, 2048], P('tp', 'fs'), may hold values from -0.109375 to 0.109375
- w_inner: bfloat16 [2048, 1024], P('fs', 'tp'), may hold values from -0.125 to 0.125
- w_bgate: bfloat16 [2048, 1024], P('fs', 'tp'), may hold values from -0.125 to 0.125
- w_cgate: bfloat16 [2048, 1024], P('fs', 'tp'), may hold values from -0.125 to 0.125
- conv_taps: float32 [3, 1024], P(None, 'tp'), may hold values from -3.5 to 3.5
- w_out: bfloat16 [1024, 2048], P('tp', 'fs'), may hold values from -0.25 to 0.25
Outputs:
- mixed: bfloat16 [4096, 2048], P(('rep', 'fs'), 'tp')
The draws below stay inside these ranges and needn't reach their ends.
All inputs are finite; a program needn't handle non-finite values.
Results may differ from the reference program's by a relative error of at most 0.02.
Values may be sent and summed in bfloat16 or wider, within the bound.
A program may use at most 128 MiB of HBM per device.

```python
import jax
import jax.numpy as jnp
from jax import lax

D = 2048
FF = 5632
CW = 1024
TAPS = 3
SEQ_LEN = 2048
TOKENS = 4096
N_TP = 2


def strengthened(values, rng, source, target, shards_of, factor):
    def block_of(position):
        return (jnp.arange(values.shape[position]) // (values.shape[position] // shards_of)).reshape((-1,) + (1,) * (values.ndim - 1 - position))

    one_side = jax.random.permutation(rng, shards_of)[block_of(target)]
    second = (block_of(target) + shards_of // 2) % shards_of
    return jnp.where((block_of(source) == one_side) | (block_of(source) == second), factor * values, values)


def levels(key, extent, pieces, least, largest):
    level, own = 1.0, jax.random.fold_in(key, 6)
    for dim, blocks in pieces:
        draws = jnp.exp(jax.random.uniform(jax.random.fold_in(own, dim), (blocks,), jnp.float32, least / len(pieces), largest / len(pieces)))
        level = level * jnp.repeat(draws, extent[dim] // blocks).reshape([-1 if axis == dim else 1 for axis in range(len(extent))])
    return level


def normal_values(rng, dims, width, limit, cuts=(), held_as=jnp.bfloat16):
    array = jax.random.normal(rng, dims, jnp.float32) * width
    if len(cuts) > 0:
        array = levels(rng, dims, cuts, -0.22, 0.18) * array
    return jnp.clip(array, min=-limit, max=limit).astype(held_as)


def noise_with(rng, extent, deviation, most, shards, heavy, dtype=jnp.bfloat16):
    values = deviation * jax.random.normal(rng, extent, jnp.float32)
    if shards:
        values = values * levels(rng, extent, shards, -0.22, 0.18)
    return jnp.clip(strengthened(values, jax.random.fold_in(rng, 3), *heavy), -most, most).astype(dtype)


def setup_inputs(seed: int = 0) -> dict:
    key_list = jax.random.split(jax.random.key(seed), 11)
    return {
        "stream": normal_values(key_list[0], (TOKENS, D), 1.0, 6.0, ((0, 16), (1, 2))),
        "norm_gains": jnp.clip(1.0 + 0.18 * jax.random.normal(key_list[1], (6, D), jnp.float32), 0.1, 1.9),
        "w_gate": normal_values(key_list[2], (D, FF), D ** -0.5, 0.125, ((0, 8), (1, 2))),
        "w_up": normal_values(key_list[3], (D, FF), D ** -0.5, 0.125, ((0, 8), (1, 2))),
        "w_down": noise_with(key_list[4], (FF, D), FF ** -0.5, 0.109375, ((0, 2), (1, 8)), (0, 1, 8, 2.0)),
        "w_inner": normal_values(key_list[5], (D, CW), D ** -0.5, 0.125, ((0, 8), (1, 2))),
        "w_bgate": normal_values(key_list[6], (D, CW), D ** -0.5, 0.125, ((0, 8), (1, 2))),
        "w_cgate": normal_values(key_list[7], (D, CW), D ** -0.5, 0.125, ((0, 8), (1, 2))),
        "conv_taps": normal_values(key_list[8], (TAPS, CW), TAPS ** -0.5, 3.5, ((1, 2),), jnp.float32),
        "w_out": noise_with(key_list[9], (CW, D), CW ** -0.5, 0.25, ((0, 2), (1, 8)), (0, 1, 8, 2.0)),
    }


EPSILON = 1e-06

def rms_scale(values):
    return values * lax.rsqrt(lax.optimization_barrier(jnp.mean(values * values, axis=1, keepdims=True)) + EPSILON)

def norm_input(current, gain):
    return (rms_scale(current.astype(jnp.float32)) * gain).astype(jnp.bfloat16)

def split_sum(hidden, weight, groups):
    columns = hidden.shape[1] // groups
    result = jnp.zeros((hidden.shape[0], weight.shape[1]), jnp.float32)
    for group in range(groups):
        partial_term = jnp.dot(hidden[:, group * columns:(group + 1) * columns], weight[group * columns:(group + 1) * columns], preferred_element_type=jnp.float32)
        rounded = lax.optimization_barrier(partial_term.astype(jnp.bfloat16))
        result = result + rounded.astype(jnp.float32)
    return result

def settle(current, branch_sum, gain, weight):
    return (current.astype(jnp.float32) + weight * (rms_scale(branch_sum) * gain)).astype(jnp.bfloat16)

def feed_forward(current, gain_in, gain_out, w_gate, w_up, w_down):
    normed = norm_input(current, gain_in)
    gate_vals = jnp.dot(normed, w_gate, preferred_element_type=jnp.float32)
    upward = jnp.dot(normed, w_up, preferred_element_type=jnp.float32)
    hidden = (jax.nn.silu(gate_vals) * upward).astype(jnp.bfloat16)
    return settle(current, split_sum(hidden, w_down, N_TP), gain_out, 0.5)

def reference(stream, norm_gains, w_gate, w_up, w_down, w_inner, w_bgate, w_cgate, conv_taps, w_out):
    first = feed_forward(stream, norm_gains[0], norm_gains[1], w_gate, w_up, w_down)
    normed = norm_input(first, norm_gains[2])
    inner = jnp.dot(normed, w_inner, preferred_element_type=jnp.float32)
    bgate = jnp.dot(normed, w_bgate, preferred_element_type=jnp.float32)
    cgate = jnp.dot(normed, w_cgate, preferred_element_type=jnp.float32)
    conv_input = (cgate * inner).reshape(-1, SEQ_LEN, CW)
    padded = jnp.pad(conv_input, ((0, 0), (TAPS - 1, 0), (0, 0)))
    conv = conv_taps[0] * padded[:, 0:SEQ_LEN]
    for tap in range(1, TAPS):
        conv = conv + conv_taps[tap] * padded[:, tap:tap + SEQ_LEN]
    gated = (bgate * conv.reshape(-1, CW)).astype(jnp.bfloat16)
    second = settle(first, split_sum(gated, w_out, N_TP), norm_gains[3], 1.0)
    return feed_forward(second, norm_gains[4], norm_gains[5], w_gate, w_up, w_down)
```

```python
import jax
import jax.numpy as jnp
from jax import lax
from jax.sharding import PartitionSpec as P

TAPS = 3
EPSILON = 1e-06


def ring_order(count):
    return list(range(0, count, 2)) + list(range(1, count, 2))[::-1]


def swap(x, axis):
    return lax.ppermute(x, axis, [(0, 1), (1, 0)])


class Ring:
    def __init__(self, own, after=None):
        count = lax.axis_size("fs")
        order = ring_order(count)
        onward = [(order[i], order[(i + 1) % count]) for i in range(count)]
        back = [(b, a) for a, b in onward]
        half = count // 2
        first, second = own, own
        if after is not None:
            first, _ = lax.optimization_barrier((own, after[0]))
            second, _ = lax.optimization_barrier((own, after[1]))
        rows = own.shape[0] // 2
        self.shards = {0: own}
        self.arrived = (own, own)
        for step in range(1, half):
            first = lax.ppermute(first, "fs", onward)
            second = lax.ppermute(second, "fs", back)
            self.shards[step] = first
            self.shards[count - step] = second
            self.arrived = (first, second)
        self.last = (
            lax.ppermute(first[:rows], "fs", onward),
            lax.ppermute(second[rows:], "fs", back),
        )
        self.shards[half] = jnp.concatenate(self.last, axis=0)
        self.sequence = [0]
        for step in range(1, half):
            self.sequence += [step, count - step]
        self.sequence += [half]

    def whole(self, origin, axis):
        shape = list(self.shards[0].shape)
        size = shape[axis]
        shape[axis] *= len(self.shards)
        result = jnp.zeros(shape, self.shards[0].dtype)
        for d in self.sequence:
            result = lax.dynamic_update_slice_in_dim(result, self.shards[d], origin[d] * size, axis)
        return result


def shards(stream, norm_gains, w_gate, w_up, w_down, w_inner, w_bgate, w_cgate, conv_taps, w_out):
    count, tp = lax.axis_size("fs"), lax.axis_size("tp")
    tp_index, rep_index, fs_index = lax.axis_index("tp"), lax.axis_index("rep"), lax.axis_index("fs")
    rows, width = stream.shape
    model_width = width * tp
    order = ring_order(count)
    places = [order.index(i) for i in range(count)]
    place = jnp.array(places, jnp.int32)[fs_index]
    origin = [
        jnp.array(order, jnp.int32)[lax.rem(place - d + count, count)] for d in range(count)
    ]

    def rep_part(w, axis):
        size = w.shape[axis] // lax.axis_size("rep")
        return lax.dynamic_slice_in_dim(w, rep_index * size, size, axis)

    def whole_features(x):
        if tp != 2:
            return lax.all_gather(x, "tp", axis=1, tiled=True)
        other = swap(x, "tp")
        mine = tp_index == 0
        return jnp.concatenate([jnp.where(mine, x, other), jnp.where(mine, other, x)], axis=1)

    def own_features(x):
        return lax.dynamic_slice_in_dim(x, tp_index * width, width, 1)

    def feature_sum(partials):
        rounded = partials.astype(jnp.bfloat16)
        if tp != 2:
            return lax.psum_scatter(rounded, "tp", scatter_dimension=1, tiled=True).astype(jnp.float32)
        theirs = lax.dynamic_slice_in_dim(rounded, (1 - tp_index) * width, width, 1)
        received = swap(theirs, "tp").astype(jnp.float32)
        return own_features(rounded).astype(jnp.float32) + received

    def norm_own(current, row):
        values = current.astype(jnp.float32)
        scaled = values * lax.rsqrt(jnp.mean(values * values, axis=1, keepdims=True) + EPSILON)
        return (scaled * norm_gains[row]).astype(jnp.bfloat16)

    def norm_other(normed):
        return whole_features(swap(own_features(normed), "rep"))

    def settle(current, own_sum, other_sum, row, weight):
        received = swap(other_sum.astype(jnp.bfloat16), "rep").astype(jnp.float32)
        branch = whole_features(own_sum + received)
        scaled = branch * lax.rsqrt(jnp.mean(branch * branch, axis=1, keepdims=True) + EPSILON)
        return (current.astype(jnp.float32) + weight * (scaled * norm_gains[row])).astype(
            jnp.bfloat16
        )

    def dot(a, b):
        return jnp.dot(a, b, preferred_element_type=jnp.float32)

    def activate(gate_vals, upward):
        return (jax.nn.silu(gate_vals) * upward).astype(jnp.bfloat16)

    current = whole_features(stream)
    normed = norm_own(current, 0)
    normed = jnp.concatenate([normed, norm_other(normed)], axis=0)

    gate_ring = Ring(rep_part(w_gate, 1))
    up_ring = Ring(rep_part(w_up, 1))
    down_own = rep_part(w_down, 0)
    hidden_units = down_own.shape[0]
    cut = max(hidden_units // 2 // 128, 1) * 128
    down_a = Ring(down_own[:cut], gate_ring.arrived)
    down_b = Ring(down_own[cut:], up_ring.arrived)
    mix_ring = Ring(
        jnp.concatenate([rep_part(w, 1) for w in (w_inner, w_bgate, w_cgate)], axis=1),
        down_a.arrived,
    )
    out_ring = Ring(rep_part(w_out, 0), down_b.arrived)

    def by_shards(ring):
        size = ring.shards[0].shape[0]
        total = None
        for d in ring.sequence:
            term = dot(lax.dynamic_slice_in_dim(normed, origin[d] * size, size, 1), ring.shards[d])
            total = term if total is None else total + term
        return total

    hidden = activate(by_shards(gate_ring), by_shards(up_ring))
    partials = jnp.zeros((2 * rows, model_width), jnp.bfloat16)
    for d in down_a.sequence:
        block = dot(hidden[:, :cut], down_a.shards[d]) + dot(hidden[:, cut:], down_b.shards[d])
        partials = lax.dynamic_update_slice_in_dim(
            partials, block.astype(jnp.bfloat16), origin[d] * block.shape[1], 1
        )
    sums = feature_sum(partials)
    first = settle(current, sums[:rows], sums[rows:], 1, 0.5)

    mix_whole, out_whole = mix_ring.whole(origin, 0), out_ring.whole(origin, 1)
    channels = mix_whole.shape[1] // 3
    taps = rep_part(conv_taps, 1)

    def mix_in(normed_mix):
        product = dot(normed_mix, mix_whole)
        inner, bgate, cgate = (product[:, i * channels : (i + 1) * channels] for i in range(3))
        return cgate * inner, bgate

    def mix_out(conv_input, bgate, earlier):
        padded = jnp.concatenate([earlier, conv_input], axis=0)
        conv = taps[0] * padded[0:rows]
        for tap in range(1, TAPS):
            conv = conv + taps[tap] * padded[tap : tap + rows]
        return feature_sum(dot((bgate * conv).astype(jnp.bfloat16), out_whole))

    normed_mix = norm_own(first, 2)
    other_mix = norm_other(normed_mix)
    own_in, own_bgate = mix_in(normed_mix)
    other_in, other_bgate = mix_in(other_mix)
    tails = jnp.concatenate([own_in[rows - (TAPS - 1) :], other_in[rows - (TAPS - 1) :]], axis=0)
    earlier = lax.ppermute(tails, "fs", [(i, i + 1) for i in range(count - 1)])
    other_sum = mix_out(other_in, other_bgate, earlier[TAPS - 1 :])
    own_sum = mix_out(own_in, own_bgate, earlier[: TAPS - 1])
    second = settle(first, own_sum, other_sum, 3, 1.0)

    gate_whole, up_whole = gate_ring.whole(origin, 0), up_ring.whole(origin, 0)
    down_whole = jnp.concatenate([down_a.whole(origin, 1), down_b.whole(origin, 1)], axis=0)

    def branch_sum(normed_rows):
        units = activate(dot(normed_rows, gate_whole), dot(normed_rows, up_whole))
        return feature_sum(dot(units, down_whole))

    normed = norm_own(second, 4)
    other_normed = norm_other(normed)
    own_sum = branch_sum(normed)
    other_sum = branch_sum(other_normed)
    return own_features(settle(second, own_sum, other_sum, 5, 0.5))


def solution(mesh):
    return jax.shard_map(
        shards,
        mesh=mesh,
        in_specs=(
            P(("rep", "fs"), "tp"),
            P(),
            P("fs", "tp"),
            P("fs", "tp"),
            P("tp", "fs"),
            P("fs", "tp"),
            P("fs", "tp"),
            P("fs", "tp"),
            P(None, "tp"),
            P("tp", "fs"),
        ),
        out_specs=P(("rep", "fs"), "tp"),
        check_vma=False,
    )
```

```python
import jax
import jax.numpy as jnp
from jax import lax
from jax.experimental import pallas as pl
from jax.experimental.pallas import tpu as pltpu
from jax.sharding import PartitionSpec as P

TAPS = 3
EPSILON = 1e-06


def ring_order(count):
    return list(range(0, count, 2)) + list(range(1, count, 2))[::-1]


def swap(x, axis):
    return lax.ppermute(x, axis, [(0, 1), (1, 0)])


def copy_block(starts, source, target):
    target[...] = source[...]


def permuted(x, starts, size):
    return pl.pallas_call(
        copy_block,
        grid_spec=pltpu.PrefetchScalarGridSpec(
            num_scalar_prefetch=1,
            grid=(len(starts),),
            in_specs=[pl.BlockSpec((x.shape[0], size), lambda i, starts: (0, starts[i]))],
            out_specs=pl.BlockSpec((x.shape[0], size), lambda i, starts: (0, i)),
        ),
        out_shape=jax.ShapeDtypeStruct(x.shape, x.dtype),
        cost_estimate=pl.CostEstimate(flops=0, bytes_accessed=2 * x.size * x.dtype.itemsize, transcendentals=0),
    )(jnp.stack(starts), x)


class Ring:
    def __init__(self, own, after=None):
        count = lax.axis_size("fs")
        order = ring_order(count)
        onward = [(order[i], order[(i + 1) % count]) for i in range(count)]
        back = [(b, a) for a, b in onward]
        half = count // 2
        first, second = own, own
        if after is not None:
            first, _ = lax.optimization_barrier((own, after[0]))
            second, _ = lax.optimization_barrier((own, after[1]))
        rows = own.shape[0] // 2
        self.shards = {0: own}
        self.arrived = self.early = (own, own)
        for step in range(1, half):
            first = lax.ppermute(first, "fs", onward)
            second = lax.ppermute(second, "fs", back)
            self.shards[step] = first
            self.shards[count - step] = second
            self.arrived = (first, second)
            if step == 1:
                self.early = self.arrived
        self.last = (
            lax.ppermute(first[:rows], "fs", onward),
            lax.ppermute(second[rows:], "fs", back),
        )
        self.shards[half] = jnp.concatenate(self.last, axis=0)
        self.sequence = [0]
        for step in range(1, half):
            self.sequence += [step, count - step]
        self.sequence += [half]

    def lined_up(self, axis):
        return jnp.concatenate([self.shards[d] for d in range(len(self.shards))], axis=axis)


def shards(stream, norm_gains, w_gate, w_up, w_down, w_inner, w_bgate, w_cgate, conv_taps, w_out):
    count, tp = lax.axis_size("fs"), lax.axis_size("tp")
    tp_index, rep_index, fs_index = lax.axis_index("tp"), lax.axis_index("rep"), lax.axis_index("fs")
    rows, width = stream.shape
    model_width = width * tp
    order = ring_order(count)
    places = [order.index(i) for i in range(count)]
    place = jnp.array(places, jnp.int32)[fs_index]
    origin = [
        jnp.array(order, jnp.int32)[lax.rem(place - d + count, count)] for d in range(count)
    ]

    behind = [
        lax.rem(place - places[i] + count, count) for i in range(count)
    ]

    def blocks(x, starts):
        size = x.shape[1] // count
        if size % 128 == 0:
            return permuted(x, starts, size)
        return jnp.concatenate(
            [lax.dynamic_slice_in_dim(x, start * size, size, 1) for start in starts], axis=1
        )

    def rep_part(w, axis):
        size = w.shape[axis] // lax.axis_size("rep")
        return lax.dynamic_slice_in_dim(w, rep_index * size, size, axis)

    def whole_features(x):
        if tp != 2:
            return lax.all_gather(x, "tp", axis=1, tiled=True)
        other = swap(x, "tp")
        mine = tp_index == 0
        return jnp.concatenate([jnp.where(mine, x, other), jnp.where(mine, other, x)], axis=1)

    def own_features(x):
        return lax.dynamic_slice_in_dim(x, tp_index * width, width, 1)

    def feature_sum(partials):
        rounded = blocks(partials.astype(jnp.bfloat16), behind)
        if tp != 2:
            return lax.psum_scatter(rounded, "tp", scatter_dimension=1, tiled=True).astype(jnp.float32)
        theirs = lax.dynamic_slice_in_dim(rounded, (1 - tp_index) * width, width, 1)
        received = swap(theirs, "tp").astype(jnp.float32)
        return own_features(rounded).astype(jnp.float32) + received

    def norm_own(current, row):
        values = current.astype(jnp.float32)
        scaled = values * lax.rsqrt(jnp.mean(values * values, axis=1, keepdims=True) + EPSILON)
        return (scaled * norm_gains[row]).astype(jnp.bfloat16)

    def norm_other(normed):
        return whole_features(swap(own_features(normed), "rep"))

    def settle(current, own_sum, other_sum, row, weight):
        received = swap(other_sum.astype(jnp.bfloat16), "rep").astype(jnp.float32)
        branch = whole_features(own_sum + received)
        scaled = branch * lax.rsqrt(jnp.mean(branch * branch, axis=1, keepdims=True) + EPSILON)
        return (current.astype(jnp.float32) + weight * (scaled * norm_gains[row])).astype(
            jnp.bfloat16
        )

    def dot(a, b):
        return jnp.dot(a, b, preferred_element_type=jnp.float32)

    def activate(gate_vals, upward):
        return (jax.nn.silu(gate_vals) * upward).astype(jnp.bfloat16)

    current = whole_features(stream)
    normed = norm_own(current, 0)
    normed = jnp.concatenate([normed, norm_other(normed)], axis=0)

    gate_ring = Ring(rep_part(w_gate, 1))
    up_ring = Ring(rep_part(w_up, 1))
    down_own = rep_part(w_down, 0)
    down_ring = Ring(down_own, gate_ring.arrived)
    mix_own = jnp.concatenate([rep_part(w, 1) for w in (w_inner, w_bgate, w_cgate)], axis=1)
    out_own = rep_part(w_out, 0)
    mix_width = mix_own.shape[1]
    mix_ring = Ring(
        jnp.concatenate([mix_own, out_own.reshape(mix_own.shape[0], -1)], axis=1), down_ring.early
    )

    def by_shards(ring):
        size = ring.shards[0].shape[0]
        total = None
        for d in ring.sequence:
            term = dot(lax.dynamic_slice_in_dim(normed, origin[d] * size, size, 1), ring.shards[d])
            total = term if total is None else total + term
        return total

    hidden = activate(by_shards(gate_ring), by_shards(up_ring))
    down_blocks = {d: dot(hidden, down_ring.shards[d]).astype(jnp.bfloat16) for d in down_ring.sequence}
    sums = feature_sum(jnp.concatenate([down_blocks[d] for d in range(count)], axis=1))
    first = settle(current, sums[:rows], sums[rows:], 1, 0.5)

    mix_whole = mix_ring.lined_up(0)[:, :mix_width]
    out_whole = jnp.concatenate(
        [mix_ring.shards[d][:, mix_width:].reshape(out_own.shape) for d in range(count)], axis=1
    )
    channels = mix_width // 3
    taps = rep_part(conv_taps, 1)

    def mix_in(normed_mix):
        product = dot(blocks(normed_mix, origin), mix_whole)
        inner, bgate, cgate = (product[:, i * channels : (i + 1) * channels] for i in range(3))
        return cgate * inner, bgate

    def mix_out(conv_input, bgate, earlier):
        padded = jnp.concatenate([earlier, conv_input], axis=0)
        conv = taps[0] * padded[0:rows]
        for tap in range(1, TAPS):
            conv = conv + taps[tap] * padded[tap : tap + rows]
        return feature_sum(dot((bgate * conv).astype(jnp.bfloat16), out_whole))

    normed_mix = norm_own(first, 2)
    other_mix = norm_other(normed_mix)
    own_in, own_bgate = mix_in(normed_mix)
    other_in, other_bgate = mix_in(other_mix)
    tails = jnp.concatenate([own_in[rows - (TAPS - 1) :], other_in[rows - (TAPS - 1) :]], axis=0)
    earlier = lax.ppermute(tails, "fs", [(i, i + 1) for i in range(count - 1)])
    other_sum = mix_out(other_in, other_bgate, earlier[TAPS - 1 :])
    own_sum = mix_out(own_in, own_bgate, earlier[: TAPS - 1])
    second = settle(first, own_sum, other_sum, 3, 1.0)

    gate_whole, up_whole = gate_ring.lined_up(0), up_ring.lined_up(0)
    down_whole = down_ring.lined_up(1)

    def units(normed_rows):
        lined = blocks(normed_rows, origin)
        return activate(dot(lined, gate_whole), dot(lined, up_whole))

    normed = norm_own(second, 4)
    other_normed = norm_other(normed)
    own_units = units(normed)
    other_sum = feature_sum(dot(units(other_normed), down_whole))
    own_sum = feature_sum(dot(own_units, down_whole))
    return own_features(settle(second, own_sum, other_sum, 5, 0.5))


def solution(mesh):
    return jax.shard_map(
        shards,
        mesh=mesh,
        in_specs=(
            P(("rep", "fs"), "tp"),
            P(),
            P("fs", "tp"),
            P("fs", "tp"),
            P("tp", "fs"),
            P("fs", "tp"),
            P("fs", "tp"),
            P("fs", "tp"),
            P(None, "tp"),
            P("tp", "fs"),
        ),
        out_specs=P(("rep", "fs"), "tp"),
        check_vma=False,
    )
```

```python
import functools

import jax
import jax.numpy as jnp
from jax import lax
from jax.experimental import pallas as pl
from jax.experimental.pallas import tpu as pltpu
from jax.sharding import PartitionSpec as P

TAPS = 3
EPSILON = 1e-06


def ring_order(count):
    return list(range(0, count, 2)) + list(range(1, count, 2))[::-1]


def swap(x, axis):
    return lax.ppermute(x, axis, [(0, 1), (1, 0)])


def copy_blocks(count, size, starts, source, target):
    for i in range(count):
        begin = pl.multiple_of(starts[i] * size, size)
        target[:, i * size : (i + 1) * size] = source[:, pl.ds(begin, size)]


def permuted(x, starts, size):
    return pl.pallas_call(
        functools.partial(copy_blocks, len(starts), size),
        in_specs=[
            pl.BlockSpec(memory_space=pltpu.SMEM),
            pl.BlockSpec(memory_space=pltpu.VMEM),
        ],
        out_specs=pl.BlockSpec(memory_space=pltpu.VMEM),
        out_shape=jax.ShapeDtypeStruct(x.shape, x.dtype),
        cost_estimate=pl.CostEstimate(flops=0, bytes_accessed=2 * x.size * x.dtype.itemsize, transcendentals=0),
        compiler_params=pltpu.CompilerParams(vmem_limit_bytes=3 * x.size * x.dtype.itemsize),
    )(jnp.stack(starts), x)


class Ring:
    def __init__(self, own, after=None):
        count = lax.axis_size("fs")
        order = ring_order(count)
        onward = [(order[i], order[(i + 1) % count]) for i in range(count)]
        back = [(b, a) for a, b in onward]
        half = count // 2
        first, second = own, own
        if after is not None:
            first, _ = lax.optimization_barrier((own, after[0]))
            second, _ = lax.optimization_barrier((own, after[1]))
        rows = own.shape[0] // 2
        self.shards = {0: own}
        self.arrived = self.early = (own, own)
        for step in range(1, half):
            first = lax.ppermute(first, "fs", onward)
            second = lax.ppermute(second, "fs", back)
            self.shards[step] = first
            self.shards[count - step] = second
            self.arrived = (first, second)
            if step == 1:
                self.early = self.arrived
        self.last = (
            lax.ppermute(first[:rows], "fs", onward),
            lax.ppermute(second[rows:], "fs", back),
        )
        self.shards[half] = jnp.concatenate(self.last, axis=0)
        self.sequence = [0]
        for step in range(1, half):
            self.sequence += [step, count - step]
        self.sequence += [half]

    def lined_up(self, axis):
        return jnp.concatenate([self.shards[d] for d in range(len(self.shards))], axis=axis)


def shards(stream, norm_gains, w_gate, w_up, w_down, w_inner, w_bgate, w_cgate, conv_taps, w_out):
    count, tp = lax.axis_size("fs"), lax.axis_size("tp")
    tp_index, rep_index, fs_index = lax.axis_index("tp"), lax.axis_index("rep"), lax.axis_index("fs")
    rows, width = stream.shape
    model_width = width * tp
    order = ring_order(count)
    places = [order.index(i) for i in range(count)]
    place = jnp.array(places, jnp.int32)[fs_index]
    origin = [
        jnp.array(order, jnp.int32)[lax.rem(place - d + count, count)] for d in range(count)
    ]

    behind = [
        lax.rem(place - places[i] + count, count) for i in range(count)
    ]

    def blocks(x, starts):
        size = x.shape[1] // count
        if size % 128 == 0:
            return permuted(x, starts, size)
        return jnp.concatenate(
            [lax.dynamic_slice_in_dim(x, start * size, size, 1) for start in starts], axis=1
        )

    def rep_part(w, axis):
        size = w.shape[axis] // lax.axis_size("rep")
        return lax.dynamic_slice_in_dim(w, rep_index * size, size, axis)

    def whole_features(x):
        if tp != 2:
            return lax.all_gather(x, "tp", axis=1, tiled=True)
        other = swap(x, "tp")
        mine = tp_index == 0
        return jnp.concatenate([jnp.where(mine, x, other), jnp.where(mine, other, x)], axis=1)

    def own_features(x):
        return lax.dynamic_slice_in_dim(x, tp_index * width, width, 1)

    def feature_sum(partials):
        rounded = blocks(partials.astype(jnp.bfloat16), behind)
        if tp != 2:
            return lax.psum_scatter(rounded, "tp", scatter_dimension=1, tiled=True).astype(jnp.float32)
        theirs = lax.dynamic_slice_in_dim(rounded, (1 - tp_index) * width, width, 1)
        received = swap(theirs, "tp").astype(jnp.float32)
        return own_features(rounded).astype(jnp.float32) + received

    def norm_own(current, row):
        values = current.astype(jnp.float32)
        scaled = values * lax.rsqrt(jnp.mean(values * values, axis=1, keepdims=True) + EPSILON)
        return (scaled * norm_gains[row]).astype(jnp.bfloat16)

    def norm_other(normed):
        return whole_features(swap(own_features(normed), "rep"))

    def settle(current, own_sum, other_sum, row, weight):
        received = swap(other_sum.astype(jnp.bfloat16), "rep").astype(jnp.float32)
        branch = whole_features(own_sum + received)
        scaled = branch * lax.rsqrt(jnp.mean(branch * branch, axis=1, keepdims=True) + EPSILON)
        return (current.astype(jnp.float32) + weight * (scaled * norm_gains[row])).astype(
            jnp.bfloat16
        )

    def dot(a, b):
        return jnp.dot(a, b, preferred_element_type=jnp.float32)

    def activate(gate_vals, upward):
        return (jax.nn.silu(gate_vals) * upward).astype(jnp.bfloat16)

    current = whole_features(stream)
    normed = norm_own(current, 0)
    normed = jnp.concatenate([normed, norm_other(normed)], axis=0)

    gate_ring = Ring(rep_part(w_gate, 1))
    up_ring = Ring(rep_part(w_up, 1))
    down_own = rep_part(w_down, 0)
    down_ring = Ring(down_own, gate_ring.arrived)
    mix_own = jnp.concatenate([rep_part(w, 1) for w in (w_inner, w_bgate, w_cgate)], axis=1)
    out_own = rep_part(w_out, 0)
    mix_width = mix_own.shape[1]
    mix_ring = Ring(
        jnp.concatenate([mix_own, out_own.reshape(mix_own.shape[0], -1)], axis=1), down_ring.early
    )

    def by_shards(ring):
        size = ring.shards[0].shape[0]
        total = None
        for d in ring.sequence:
            term = dot(lax.dynamic_slice_in_dim(normed, origin[d] * size, size, 1), ring.shards[d])
            total = term if total is None else total + term
        return total

    hidden = activate(by_shards(gate_ring), by_shards(up_ring))
    down_blocks = {d: dot(hidden, down_ring.shards[d]).astype(jnp.bfloat16) for d in down_ring.sequence}
    sums = feature_sum(jnp.concatenate([down_blocks[d] for d in range(count)], axis=1))
    first = settle(current, sums[:rows], sums[rows:], 1, 0.5)

    mix_whole = mix_ring.lined_up(0)[:, :mix_width]
    out_whole = jnp.concatenate(
        [mix_ring.shards[d][:, mix_width:].reshape(out_own.shape) for d in range(count)], axis=1
    )
    channels = mix_width // 3
    taps = rep_part(conv_taps, 1)

    def mix_in(normed_mix):
        product = dot(blocks(normed_mix, origin), mix_whole)
        inner, bgate, cgate = (product[:, i * channels : (i + 1) * channels] for i in range(3))
        return cgate * inner, bgate

    def mix_out(conv_input, bgate, earlier):
        padded = jnp.concatenate([earlier, conv_input], axis=0)
        conv = taps[0] * padded[0:rows]
        for tap in range(1, TAPS):
            conv = conv + taps[tap] * padded[tap : tap + rows]
        return feature_sum(dot((bgate * conv).astype(jnp.bfloat16), out_whole))

    normed_mix = norm_own(first, 2)
    other_mix = norm_other(normed_mix)
    own_in, own_bgate = mix_in(normed_mix)
    other_in, other_bgate = mix_in(other_mix)
    tails = jnp.concatenate([own_in[rows - (TAPS - 1) :], other_in[rows - (TAPS - 1) :]], axis=0)
    earlier = lax.ppermute(tails, "fs", [(i, i + 1) for i in range(count - 1)])
    other_sum = mix_out(other_in, other_bgate, earlier[TAPS - 1 :])
    own_sum = mix_out(own_in, own_bgate, earlier[: TAPS - 1])
    second = settle(first, own_sum, other_sum, 3, 1.0)

    gate_whole, up_whole = gate_ring.lined_up(0), up_ring.lined_up(0)
    down_whole = down_ring.lined_up(1)

    def units(normed_rows):
        lined = blocks(normed_rows, origin)
        return activate(dot(lined, gate_whole), dot(lined, up_whole))

    normed = norm_own(second, 4)
    other_normed = norm_other(normed)
    own_units = units(normed)
    other_sum = feature_sum(dot(units(other_normed), down_whole))
    own_sum = feature_sum(dot(own_units, down_whole))
    return own_features(settle(second, own_sum, other_sum, 5, 0.5))


def solution(mesh):
    return jax.shard_map(
        shards,
        mesh=mesh,
        in_specs=(
            P(("rep", "fs"), "tp"),
            P(),
            P("fs", "tp"),
            P("fs", "tp"),
            P("tp", "fs"),
            P("fs", "tp"),
            P("fs", "tp"),
            P("fs", "tp"),
            P(None, "tp"),
            P("tp", "fs"),
        ),
        out_specs=P(("rep", "fs"), "tp"),
        check_vma=False,
    )
```
